32 devices in a mesh: grp: 2 (over x), ep: 16 (over z, y, core).
Axes of the slice: x: 2, y: 2, z: 4, core: 2. Of those that a mesh axis runs over, the one named last changes fastest.
Arguments:
- tokens: bfloat16 [1024, 2048], P(('grp', 'ep')), parts along dimension 0, may hold values from -6 to 6
- norm_gain: float32 [2048], replicated, may hold values from 0.1 to 1.9
- routing: int32 [1024, 8], P(('grp', 'ep')), parts along dimension 0, may hold values from 0 to 15, all different within a row; in each aligned block of 32 rows (0 to 31, 32 to 63, ...) at most 32 rows name the same one
- gates: float32 [1024, 8], P(('grp', 'ep')), parts along dimension 0, may hold values from 0.05 to 0.6
- w_gate: bfloat16 [16, 2048, 512], P('ep'), may hold values from -0.125 to 0.125
- w_up: bfloat16 [16, 2048, 512], P('ep'), may hold values from -0.125 to 0.125
- w_down: bfloat16 [16, 512, 2048], P('ep'), may hold values from -0.25 to 0.25
- shared_gate: bfloat16 [2048, 512], replicated, may hold values from -0.125 to 0.125
- shared_up: bfloat16 [2048, 512], replicated, may hold values from -0.125 to 0.125
- shared_down: bfloat16 [512, 2048], replicated, may hold values from -0.25 to 0.25
Outputs:
- mixed: bfloat16 [1024, 2048], P(('grp', 'ep')), parts along dimension 0
The draws below stay inside these ranges and needn't reach their ends.
There are 2 independent parts, one for each index of `grp`. The reference program is written for one: setup_inputs(seed, part) draws one part's arguments, and reference() takes and returns one part's arrays. A program takes and returns all parts, laid end to end along the dimension named above; an argument that names none is the same for every part. Nothing has to cross between parts.
Inputs may be any that keep to these rules, and one draw needn't show every extreme that they name: `routing`: within the 32 rows of one device no expert is named by more than 32 rows, and in every draw some expert is named by exactly 32 rows of some device; each row names 8 different experts.
All inputs are finite; a program needn't handle non-finite values.
Results may differ from the reference program's by a relative error of at most 0.0067.
Values may be sent and summed in bfloat16 or wider, within the bound.
No kernel may reach another device: no remote copies, remote signals or barrier semaphores. Data moves between devices by JAX's collectives and lax.ppermute only.
A program may use at most 128 MiB of HBM per device.

```python
import math
import jax
import jax.numpy as jnp
import numpy as np
from jax import lax

D = 2048
FF = 512
SHARED_FF = 512
TOP_K = 8
TOK_DEV = 32
EXPERTS = 16
TOKENS = 512
SLOTS = 32
N_EP = 16


def steps_of(key, extent, pieces, least, high):
    factor_of, own = 1.0, jax.random.fold_in(key, 6)
    for dim, shards_of in pieces:
        heights = jnp.exp(jax.random.uniform(jax.random.fold_in(own, dim), (shards_of,), jnp.float32, least / len(pieces), high / len(pieces)))
        factor_of = factor_of * jnp.repeat(heights, extent[dim] // shards_of).reshape([-1 if axis == dim else 1 for axis in range(len(extent))])
    return factor_of


def routed_block(key, own, number, rows, amount, top, reach, skew):
    ranking = jax.random.permutation(key, amount)
    crowded, common = load_shares(amount, rows * top, reach, skew, True), load_shares(amount, rows * top, reach, skew, False)
    places = jnp.arange(amount)

    def named(sizes, rotation):
        used = int((sizes > 0).sum())
        fixed = max(1, used // 4)
        passed = fixed + (places - fixed + rotation * (used - fixed)) % max(1, amount - fixed)
        return jnp.zeros((amount,), jnp.int32).at[ranking[jnp.where(places < fixed, places, passed)]].set(jnp.asarray(sizes, jnp.int32))

    sizes = jnp.where(number % 4 == 0, named(crowded, number // 4), named(common, number - number // 4 - 1))
    mixed = jax.random.permutation(jax.random.fold_in(own, 3), amount)
    giver, receiver = mixed[0:amount // 2 * 2:2], mixed[1:amount // 2 * 2:2]
    slack = jnp.minimum(sizes[giver] - 1, reach - sizes[receiver]) // 2
    slack = jnp.where((giver == ranking[0]) | (receiver == ranking[0]) | (sizes[receiver] == 0), 0, jnp.maximum(slack, 0))
    passed = jax.random.randint(jax.random.fold_in(own, 4), (amount // 2,), 0, 1 << 20) % (slack + 1)
    sizes = sizes.at[giver].add(-passed).at[receiver].add(passed)
    labels = jnp.searchsorted(jnp.cumsum(sizes), jnp.arange(rows * top), side="right").astype(jnp.int32)
    grid = labels.reshape(top, rows).T
    grid = grid[jax.random.permutation(jax.random.fold_in(own, 1), rows)]
    rotation = jax.random.randint(jax.random.fold_in(own, 2), (rows, 1), 0, top)
    return jnp.take_along_axis(grid, (jnp.arange(top)[None, :] + rotation) % top, axis=1)


def load_shares(amount, total, limit, skew, full):
    loads = [(1 << 20) // math.isqrt(standing ** skew) + 1 for standing in range(1, amount + 1)]
    largest = limit if full else min(limit, max(-(-total // amount), total * loads[0] // sum(loads)))
    least = 1 if total - largest >= amount - 1 else 0
    given, surplus = [largest] + [least] * (amount - 1), total - largest - least * (amount - 1)
    while surplus > 0:
        candidates = [i for i in range(1, amount) if given[i] < largest] or [i for i in range(1, amount) if given[i] < limit]
        mass, budget = sum([loads[i] for i in candidates]), surplus
        for i in candidates:
            more = min(limit - given[i], max(1, budget * loads[i] // mass), surplus)
            given[i] = given[i] + more
            surplus = surplus - more
    return np.array(given)


def bell_draw(own_key, shape, width, bound, split=(), kind=jnp.bfloat16):
    values = jax.random.normal(own_key, shape, jnp.float32) * width
    if len(split) > 0:
        values = steps_of(own_key, shape, split, -0.22, 0.18) * values
    return jnp.clip(values, min=-bound, max=bound).astype(kind)


def setup_inputs(seed: int = 0, part: int = 0) -> dict:
    key_of = jax.random.split(jax.random.key(seed), 11)
    own_keys = jax.random.split(jax.random.fold_in(key_of[10], part), 11)
    tokens = bell_draw(own_keys[0], (TOKENS, D), 1.0, 6.0, ((0, 16),))
    norm_gain = jnp.clip(1.0 + 0.18 * jax.random.normal(key_of[1], (D,), jnp.float32), 0.1, 1.9)
    routing_keys = jax.random.split(jax.random.fold_in(own_keys[2], 1), TOKENS // TOK_DEV)
    routing_turns = jax.random.permutation(jax.random.fold_in(own_keys[2], 3), TOKENS // TOK_DEV)
    routing = jax.vmap(lambda own, number: routed_block(jax.random.fold_in(own_keys[2], 2), own, number, TOK_DEV, EXPERTS, TOP_K, SLOTS, 2))(routing_keys, routing_turns).reshape((TOKENS, TOP_K))
    gates = jnp.clip(jnp.exp(math.log(0.6) - 2.4849067 * jax.random.uniform(own_keys[3], (TOKENS, TOP_K), jnp.float32) ** steps_of(own_keys[3], (TOKENS, TOP_K), ((0, 16),), -0.2, 0.2)), 0.05, 0.6)
    w_gate = bell_draw(key_of[4], (EXPERTS, D, FF), D ** -0.5, 0.125, ((0, 16),))
    w_up = bell_draw(key_of[5], (EXPERTS, D, FF), D ** -0.5, 0.125, ((0, 16),))
    w_down = bell_draw(key_of[6], (EXPERTS, FF, D), FF ** -0.5, 0.25, ((0, 16),))
    shared_gate = bell_draw(key_of[7], (D, SHARED_FF), D ** -0.5, 0.125)
    shared_up = bell_draw(key_of[8], (D, SHARED_FF), D ** -0.5, 0.125)
    shared_down = bell_draw(key_of[9], (SHARED_FF, D), SHARED_FF ** -0.5, 0.25)
    return dict(tokens=tokens, norm_gain=norm_gain, routing=routing, gates=gates, w_gate=w_gate, w_up=w_up, w_down=w_down, shared_gate=shared_gate, shared_up=shared_up, shared_down=shared_down)


epsilon = 1e-06

def rms_normed(tokens, norm_gain):
    floats = tokens.astype(jnp.float32)
    scale_inv = lax.rsqrt(lax.optimization_barrier(jnp.mean(floats * floats, axis=-1, keepdims=True)) + epsilon)
    return (floats * scale_inv * norm_gain.astype(jnp.float32)).astype(jnp.bfloat16)

def reference(tokens, norm_gain, routing, gates, w_gate, w_up, w_down, shared_gate, shared_up, shared_down):
    normed = rms_normed(tokens, norm_gain)
    shared_hidden = (jax.nn.silu(jnp.dot(normed, shared_gate, preferred_element_type=jnp.float32)) * jnp.dot(normed, shared_up, preferred_element_type=jnp.float32)).astype(jnp.bfloat16)
    shared_out = jnp.dot(shared_hidden, shared_down, preferred_element_type=jnp.float32)
    capacity = N_EP * SLOTS
    token_total = normed.shape[0]
    positions = jnp.arange(token_total, dtype=jnp.int32)

    def visit(totals, inputs):
        gate_part, up_part, down_part, expert = inputs
        chosen_pairs = routing == expert
        chosen = jnp.any(chosen_pairs, axis=1)
        weights = lax.optimization_barrier(jnp.sum(jnp.where(chosen_pairs, gates, jnp.zeros_like(gates)), axis=1))
        ranked = jnp.cumsum(chosen.astype(jnp.int32)) - 1
        target = jnp.where(chosen, ranked, capacity).astype(jnp.int32)
        picks = jnp.zeros((capacity,), jnp.int32).at[target].set(positions, mode='drop')
        live = jnp.zeros((capacity,), weights.dtype).at[target].set(weights, mode='drop')
        picked = normed[picks]
        hidden = (jax.nn.silu(jnp.dot(picked, gate_part, preferred_element_type=jnp.float32)) * jnp.dot(picked, up_part, preferred_element_type=jnp.float32)).astype(jnp.bfloat16)
        outputs = jnp.dot(hidden, down_part, preferred_element_type=jnp.float32).astype(jnp.bfloat16)
        totals = totals.at[picks].add(live[:, None] * outputs.astype(jnp.float32))
        return (totals, None)
    start = jnp.zeros((token_total, normed.shape[1]), jnp.float32)
    routed, _ = lax.scan(visit, start, (w_gate, w_up, w_down, jnp.arange(w_gate.shape[0], dtype=jnp.int32)))
    return (shared_out + routed).astype(jnp.bfloat16)
```

```python
import jax
import jax.numpy as jnp
from jax import lax
from jax.sharding import PartitionSpec as P

epsilon = 1e-06


def rms_normed(tokens, norm_gain):
    floats = tokens.astype(jnp.float32)
    scale_inv = lax.rsqrt(jnp.mean(floats * floats, axis=-1, keepdims=True) + epsilon)
    return (floats * scale_inv * norm_gain).astype(jnp.bfloat16)


def dense_gates(routing, gates, expert_count):
    ids = jnp.arange(expert_count, dtype=jnp.int32)
    matches = routing[..., None] == ids
    return jnp.sum(jnp.where(matches, gates[..., None], 0.0), axis=1)


def split3(values):
    def cut(v):
        return lax.reduce_precision(v, 8, 7)

    high = cut(values)
    middle = cut(values - high)
    low = values - high - middle
    return jnp.concatenate([high, middle, low], axis=1).astype(jnp.bfloat16)


def body(
    tokens, norm_gain, routing, gates, w_gate, w_up, w_down, shared_gate, shared_up, shared_down
):
    normed = rms_normed(tokens, norm_gain)
    width = normed.shape[1]
    local_count = w_gate.shape[0]
    ep_size = lax.axis_size("ep")
    expert_count = local_count * ep_size
    parts = split3(dense_gates(routing, gates, expert_count))
    parts = jnp.pad(parts, ((0, 0), (0, -parts.shape[1] % 128)))
    gathered = lax.all_gather(
        jnp.concatenate([normed, parts], axis=1), "ep", axis=0, tiled=True
    )
    shared_hidden = (
        jax.nn.silu(jnp.dot(normed, shared_gate, preferred_element_type=jnp.float32))
        * jnp.dot(normed, shared_up, preferred_element_type=jnp.float32)
    ).astype(jnp.bfloat16)
    shared_out = jnp.dot(shared_hidden, shared_down, preferred_element_type=jnp.float32)
    every = gathered[:, :width]
    split = gathered[:, width:].astype(jnp.float32)
    my_index = lax.axis_index("ep")
    total = None
    for i in range(local_count):
        expert = my_index * local_count + i
        columns = jnp.arange(split.shape[1], dtype=jnp.int32)
        mine = (columns % expert_count == expert) & (columns < 3 * expert_count)
        weight = jnp.sum(jnp.where(mine, split, 0.0), axis=1, keepdims=True)
        gate_act = jnp.dot(every, w_gate[i], preferred_element_type=jnp.float32)
        up_act = jnp.dot(every, w_up[i], preferred_element_type=jnp.float32)
        hidden = (jax.nn.silu(gate_act) * up_act).astype(jnp.bfloat16)
        out = jnp.dot(hidden, w_down[i], preferred_element_type=jnp.float32)
        out = weight * out
        total = out if total is None else total + out
    routed = lax.psum_scatter(
        total.astype(jnp.bfloat16), "ep", scatter_dimension=0, tiled=True
    )
    return (shared_out + routed.astype(jnp.float32)).astype(jnp.bfloat16)


def solution(mesh):
    placed = (
        P(("grp", "ep"), None),
        P(),
        P(("grp", "ep"), None),
        P(("grp", "ep"), None),
        P("ep", None, None),
        P("ep", None, None),
        P("ep", None, None),
        P(),
        P(),
        P(),
    )
    return jax.shard_map(
        body, mesh=mesh, in_specs=placed, out_specs=P(("grp", "ep"), None), check_vma=False
    )
```

```python
import jax
import jax.numpy as jnp
from jax import lax
from jax.sharding import PartitionSpec as P

epsilon = 1e-06


def rms_normed(tokens, norm_gain):
    floats = tokens.astype(jnp.float32)
    scale_inv = lax.rsqrt(jnp.mean(floats * floats, axis=-1, keepdims=True) + epsilon)
    return (floats * scale_inv * norm_gain).astype(jnp.bfloat16)


def dense_gates(routing, gates, expert_count):
    ids = jnp.arange(expert_count, dtype=jnp.int32)
    matches = routing[..., None] == ids
    return jnp.sum(jnp.where(matches, gates[..., None], 0.0), axis=1)


def split3(values):
    def cut(v):
        return lax.reduce_precision(v, 8, 7)

    high = cut(values)
    middle = cut(values - high)
    low = values - high - middle
    return jnp.concatenate([high, middle, low], axis=1).astype(jnp.bfloat16)


def partner_send(value, bit, size):
    return lax.ppermute(value, "ep", [(i, i ^ (1 << bit)) for i in range(size)])


def bit_orders(bit_count):
    first = list(range(bit_count))
    second = list(first)
    if bit_count > 2:
        second[1], second[2] = second[2], second[1]
    return first, second


def spread(shard, order, size):
    bit_count = len(order)
    grown = shard.reshape((1,) * bit_count + shard.shape)
    for bit in reversed(order[1:]):
        grown = jnp.concatenate([grown, partner_send(grown, bit, size)], axis=bit)
    return grown, partner_send(grown, order[0], size)


def fold(kept, sent, order, size):
    kept = kept + partner_send(sent.astype(jnp.bfloat16), order[0], size).astype(jnp.float32)
    for bit in order[1:]:
        leave = lax.slice_in_dim(kept, 1, 2, axis=bit).astype(jnp.bfloat16)
        stay = lax.slice_in_dim(kept, 0, 1, axis=bit)
        kept = stay + partner_send(leave, bit, size).astype(jnp.float32)
    return kept.reshape(kept.shape[-2:])


def body(
    tokens, norm_gain, routing, gates, w_gate, w_up, w_down, shared_gate, shared_up, shared_down
):
    normed = rms_normed(tokens, norm_gain)
    tok_count, width = normed.shape
    half = width // 2
    local_count = w_gate.shape[0]
    size = lax.axis_size("ep")
    bit_count = size.bit_length() - 1
    expert_count = local_count * size
    parts = split3(dense_gates(routing, gates, expert_count))
    parts = jnp.pad(parts, ((0, 0), (0, -parts.shape[1] % 128)))
    order_a, order_b = bit_orders(bit_count)
    grown_a = spread(jnp.concatenate([normed[:, :half], parts], axis=1), order_a, size)
    grown_b = spread(normed[:, half:], order_b, size)
    shared_hidden = (
        jax.nn.silu(jnp.dot(normed, shared_gate, preferred_element_type=jnp.float32))
        * jnp.dot(normed, shared_up, preferred_element_type=jnp.float32)
    ).astype(jnp.bfloat16)
    shared_out = jnp.dot(shared_hidden, shared_down, preferred_element_type=jnp.float32)
    my_index = lax.axis_index("ep")
    columns = jnp.arange(parts.shape[1], dtype=jnp.int32)
    totals = []
    for piece_a, piece_b in zip(grown_a, grown_b):
        lead = piece_b.shape[:-1]
        flat_a = piece_a.reshape(-1, piece_a.shape[-1])
        flat_b = piece_b.reshape(-1, piece_b.shape[-1])
        every = jnp.concatenate([flat_a[:, :half], flat_b], axis=1)
        split = flat_a[:, half:].astype(jnp.float32)
        total = None
        for i in range(local_count):
            expert = my_index * local_count + i
            mine = (columns % expert_count == expert) & (columns < 3 * expert_count)
            weight = jnp.sum(jnp.where(mine, split, 0.0), axis=1, keepdims=True)
            gate_act = jnp.dot(every, w_gate[i], preferred_element_type=jnp.float32)
            up_act = jnp.dot(every, w_up[i], preferred_element_type=jnp.float32)
            hidden = (jax.nn.silu(gate_act) * up_act).astype(jnp.bfloat16)
            out = jnp.dot(hidden, w_down[i], preferred_element_type=jnp.float32)
            out = weight * out
            total = out if total is None else total + out
        totals.append((total[:, :half].reshape(lead + (half,)), total[:, half:].reshape(lead + (width - half,))))
    (kept_a, kept_b), (sent_a, sent_b) = totals
    routed = jnp.concatenate(
        [fold(kept_a, sent_a, order_a, size), fold(kept_b, sent_b, order_b, size)], axis=1
    )
    return (shared_out + routed).astype(jnp.bfloat16)


def solution(mesh):
    placed = (
        P(("grp", "ep"), None),
        P(),
        P(("grp", "ep"), None),
        P(("grp", "ep"), None),
        P("ep", None, None),
        P("ep", None, None),
        P("ep", None, None),
        P(),
        P(),
        P(),
    )
    return jax.shard_map(
        body, mesh=mesh, in_specs=placed, out_specs=P(("grp", "ep"), None), check_vma=False
    )
```

```python
import jax
import jax.numpy as jnp
from jax import lax
from jax.sharding import PartitionSpec as P

epsilon = 1e-06


def rms_normed(tokens, norm_gain):
    floats = tokens.astype(jnp.float32)
    scale_inv = lax.rsqrt(jnp.mean(floats * floats, axis=-1, keepdims=True) + epsilon)
    return (floats * scale_inv * norm_gain).astype(jnp.bfloat16)


def dense_gates(routing, gates, expert_count):
    ids = jnp.arange(expert_count, dtype=jnp.int32)
    matches = routing[..., None] == ids
    return jnp.sum(jnp.where(matches, gates[..., None], 0.0), axis=1)


def split3(values):
    def cut(v):
        return lax.reduce_precision(v, 8, 7)

    high = cut(values)
    middle = cut(values - high)
    low = values - high - middle
    return jnp.concatenate([high, middle, low], axis=1).astype(jnp.bfloat16)


def partner_send(value, bit, size):
    return lax.ppermute(value, "ep", [(i, i ^ (1 << bit)) for i in range(size)])


def doubled(grown, bit, size):
    return jnp.concatenate([grown, partner_send(grown, bit, size)], axis=bit)


def halved(kept, bit, size):
    leave = lax.slice_in_dim(kept, 1, 2, axis=bit).astype(jnp.bfloat16)
    stay = lax.slice_in_dim(kept, 0, 1, axis=bit)
    return stay + partner_send(leave, bit, size).astype(jnp.float32)


def spread(shard, size, bit_count, cut, aside):
    grown = shard.reshape((1,) * bit_count + shard.shape)
    for bit in range(bit_count - 1, 2, -1):
        grown = doubled(grown, bit, size)
    if bit_count > 2:
        left, right = grown[..., :cut], grown[..., cut:]
        left, right = doubled(left, 2, size), doubled(right, 1, size)
        left, right, aside = lax.optimization_barrier((left, right, aside))
        left, right = doubled(left, 1, size), doubled(right, 2, size)
        grown = jnp.concatenate([left, right], axis=-1)
    elif bit_count > 1:
        grown = doubled(grown, 1, size)
    return grown, partner_send(grown, 0, size), aside


def fold(kept, sent, size, bit_count, cut):
    kept = kept + partner_send(sent.astype(jnp.bfloat16), 0, size).astype(jnp.float32)
    if bit_count > 2:
        left, right = kept[..., :cut], kept[..., cut:]
        left, right = halved(left, 1, size), halved(right, 2, size)
        left, right = halved(left, 2, size), halved(right, 1, size)
        kept = jnp.concatenate([left, right], axis=-1)
    elif bit_count > 1:
        kept = halved(kept, 1, size)
    for bit in range(3, bit_count):
        kept = halved(kept, bit, size)
    return kept.reshape(kept.shape[-2:])


def body(
    tokens, norm_gain, routing, gates, w_gate, w_up, w_down, shared_gate, shared_up, shared_down
):
    normed = rms_normed(tokens, norm_gain)
    width = normed.shape[1]
    half = width // 2
    local_count = w_gate.shape[0]
    size = lax.axis_size("ep")
    bit_count = size.bit_length() - 1
    expert_count = local_count * size
    parts = split3(dense_gates(routing, gates, expert_count))
    parts = jnp.pad(parts, ((0, 0), (0, -parts.shape[1] % 128)))
    shared_hidden = (
        jax.nn.silu(jnp.dot(normed, shared_gate, preferred_element_type=jnp.float32))
        * jnp.dot(normed, shared_up, preferred_element_type=jnp.float32)
    ).astype(jnp.bfloat16)
    shared_out = jnp.dot(shared_hidden, shared_down, preferred_element_type=jnp.float32)
    pieces = spread(
        jnp.concatenate([normed, parts], axis=1), size, bit_count, half, shared_out
    )
    shared_out = pieces[2]
    my_index = lax.axis_index("ep")
    columns = jnp.arange(parts.shape[1], dtype=jnp.int32)
    totals = []
    for piece in pieces[:2]:
        lead = piece.shape[:-1]
        flat = piece.reshape(-1, piece.shape[-1])
        every = flat[:, :width]
        split = flat[:, width:].astype(jnp.float32)
        total = None
        for i in range(local_count):
            expert = my_index * local_count + i
            mine = (columns % expert_count == expert) & (columns < 3 * expert_count)
            weight = jnp.sum(jnp.where(mine, split, 0.0), axis=1, keepdims=True)
            gate_act = jnp.dot(every, w_gate[i], preferred_element_type=jnp.float32)
            up_act = jnp.dot(every, w_up[i], preferred_element_type=jnp.float32)
            hidden = (jax.nn.silu(gate_act) * up_act).astype(jnp.bfloat16)
            out = jnp.dot(hidden, w_down[i], preferred_element_type=jnp.float32)
            out = weight * out
            total = out if total is None else total + out
        totals.append(total.reshape(lead + (width,)))
    routed = fold(totals[0], totals[1], size, bit_count, half)
    return (shared_out + routed).astype(jnp.bfloat16)


def solution(mesh):
    placed = (
        P(("grp", "ep"), None),
        P(),
        P(("grp", "ep"), None),
        P(("grp", "ep"), None),
        P("ep", None, None),
        P("ep", None, None),
        P("ep", None, None),
        P(),
        P(),
        P(),
    )
    return jax.shard_map(
        body, mesh=mesh, in_specs=placed, out_specs=P(("grp", "ep"), None), check_vma=False
    )
```

```python
import jax
import jax.numpy as jnp
from jax import lax
from jax.sharding import PartitionSpec as P

epsilon = 1e-06


def rms_normed(tokens, norm_gain):
    floats = tokens.astype(jnp.float32)
    scale_inv = lax.rsqrt(jnp.mean(floats * floats, axis=-1, keepdims=True) + epsilon)
    return (floats * scale_inv * norm_gain).astype(jnp.bfloat16)


def dense_gates(routing, gates, expert_count):
    ids = jnp.arange(expert_count, dtype=jnp.int32)
    matches = routing[..., None] == ids
    return jnp.sum(jnp.where(matches, gates[..., None], 0.0), axis=1)


def split3(values):
    def cut(v):
        return lax.reduce_precision(v, 8, 7)

    high = cut(values)
    middle = cut(values - high)
    low = values - high - middle
    return jnp.concatenate([high, middle, low], axis=1).astype(jnp.bfloat16)


def partner_send(value, bit, size):
    return lax.ppermute(value, "ep", [(i, i ^ (1 << bit)) for i in range(size)])


def doubled(grown, bit, size):
    return jnp.concatenate([grown, partner_send(grown, bit, size)], axis=bit)


def halved(kept, bit, size):
    leave = lax.slice_in_dim(kept, 1, 2, axis=bit).astype(jnp.bfloat16)
    stay = lax.slice_in_dim(kept, 0, 1, axis=bit)
    return stay + partner_send(leave, bit, size).astype(jnp.float32)


def spread(shard, size, bit_count, cut, aside):
    grown = shard.reshape((1,) * bit_count + shard.shape)
    for bit in range(bit_count - 1, 2, -1):
        grown = doubled(grown, bit, size)
    if bit_count > 2:
        left, right = grown[..., :cut], grown[..., cut:]
        left, right = doubled(left, 2, size), doubled(right, 1, size)
        left, right, aside = lax.optimization_barrier((left, right, aside))
        left, right = doubled(left, 1, size), doubled(right, 2, size)
        grown = jnp.concatenate([left, right], axis=-1)
    elif bit_count > 1:
        grown = doubled(grown, 1, size)
    return grown, partner_send(grown, 0, size), aside


def fold(kept, sent, size, bit_count, cut):
    kept = kept + partner_send(sent.astype(jnp.bfloat16), 0, size).astype(jnp.float32)
    if bit_count > 2:
        left, right = kept[..., :cut], kept[..., cut:]
        left, right = halved(left, 1, size), halved(right, 2, size)
        left, right = halved(left, 2, size), halved(right, 1, size)
        kept = jnp.concatenate([left, right], axis=-1)
    elif bit_count > 1:
        kept = halved(kept, 1, size)
    for bit in range(3, bit_count):
        kept = halved(kept, bit, size)
    return kept.reshape(kept.shape[-2:])


def body(
    tokens, norm_gain, routing, gates, w_gate, w_up, w_down, shared_gate, shared_up, shared_down
):
    normed = rms_normed(tokens, norm_gain)
    width = normed.shape[1]
    half = width // 2
    local_count = w_gate.shape[0]
    size = lax.axis_size("ep")
    bit_count = size.bit_length() - 1
    expert_count = local_count * size
    parts = split3(dense_gates(routing, gates, expert_count))
    parts = jnp.pad(parts, ((0, 0), (0, -parts.shape[1] % 128)))
    shared_hidden = (
        jax.nn.silu(jnp.dot(normed, shared_gate, preferred_element_type=jnp.float32))
        * jnp.dot(normed, shared_up, preferred_element_type=jnp.float32)
    ).astype(jnp.bfloat16)
    shared_out = jnp.dot(shared_hidden, shared_down, preferred_element_type=jnp.float32)
    pieces = spread(
        jnp.concatenate([normed, parts], axis=1), size, bit_count, half, shared_out
    )
    shared_out = pieces[2]
    my_index = lax.axis_index("ep")
    columns = jnp.arange(parts.shape[1], dtype=jnp.int32)

    def hidden_of(piece):
        every = piece.reshape(-1, piece.shape[-1])[:, :width]
        rows = []
        for i in range(local_count):
            gate_act = jnp.dot(every, w_gate[i], preferred_element_type=jnp.float32)
            up_act = jnp.dot(every, w_up[i], preferred_element_type=jnp.float32)
            rows.append((jax.nn.silu(gate_act) * up_act).astype(jnp.bfloat16))
        return rows

    def weighted_of(piece, hidden):
        split = piece.reshape(-1, piece.shape[-1])[:, width:].astype(jnp.float32)
        total = None
        for i in range(local_count):
            expert = my_index * local_count + i
            mine = (columns % expert_count == expert) & (columns < 3 * expert_count)
            weight = jnp.sum(jnp.where(mine, split, 0.0), axis=1, keepdims=True)
            out = weight * jnp.dot(hidden[i], w_down[i], preferred_element_type=jnp.float32)
            total = out if total is None else total + out
        return total.reshape(piece.shape[:-1] + (width,))

    own, received = pieces[0], pieces[1]
    own_hidden = hidden_of(own)
    own_hidden, received = lax.optimization_barrier((own_hidden, received))
    sent = weighted_of(received, hidden_of(received))
    totals = [weighted_of(own, own_hidden), sent]
    routed = fold(totals[0], totals[1], size, bit_count, half)
    return (shared_out + routed).astype(jnp.bfloat16)


def solution(mesh):
    placed = (
        P(("grp", "ep"), None),
        P(),
        P(("grp", "ep"), None),
        P(("grp", "ep"), None),
        P("ep", None, None),
        P("ep", None, None),
        P("ep", None, None),
        P(),
        P(),
        P(),
    )
    return jax.shard_map(
        body, mesh=mesh, in_specs=placed, out_specs=P(("grp", "ep"), None), check_vma=False
    )
```
